32 devices in a mesh: ep: 8 (over z, y), tp: 4 (over x, core).
Axes of the slice: x: 2, y: 2, z: 4, core: 2. Of those that a mesh axis runs over, the one named last changes fastest.
Arguments:
- hidden_in: bfloat16 [128, 1024], P('ep'), may hold values from -6 to 6
- prior_state: float32 [128, 8, 128, 128], P('ep', 'tp'), may hold values from -4 to 4
- mix_gain: float32 [1024], replicated, may hold values from 0.1 to 1.9
- query_w: bfloat16 [1024, 1024], P(None, 'tp'), may hold values from -0.1875 to 0.1875
- key_w: bfloat16 [1024, 1024], P(None, 'tp'), may hold values from -0.1875 to 0.1875
- value_w: bfloat16 [1024, 1024], P(None, 'tp'), may hold values from -0.1875 to 0.1875
- decay_w: bfloat16 [1024, 8], P(None, 'tp'), may hold values from -0.1875 to 0.1875
- beta_w: bfloat16 [1024, 8], P(None, 'tp'), may hold values from -0.1875 to 0.1875
- decay_rate: float32 [8], P('tp'), may hold values from 0.05 to 3
- head_gain: float32 [128], replicated, may hold values from 0.1 to 1.9
- out_w: bfloat16 [1024, 1024], P('tp'), may hold values from -0.1875 to 0.1875
- ffn_gain: float32 [1024], replicated, may hold values from 0.1 to 1.9
- expert_ids: int32 [128, 2], P('ep'), may hold values from 0 to 7, all different within a row; in each aligned block of 16 rows (0 to 15, 16 to 31, ...) at most 10 rows name the same one
- group_share: float32 [128], P('ep'), may hold values from 0.3 to 1
- expert_share: float32 [128, 2], P('ep'), may hold values from 0.1 to 1
- expert_gate: bfloat16 [8, 1024, 512], P('ep', None, 'tp'), may hold values from -0.1875 to 0.1875
- expert_up: bfloat16 [8, 1024, 512], P('ep', None, 'tp'), may hold values from -0.1875 to 0.1875
- expert_down: bfloat16 [8, 512, 1024], P('ep', 'tp'), may hold values from -0.25 to 0.25
- dense_gate: bfloat16 [4096, 1024], P('ep', 'tp'), may hold values from -0.1875 to 0.1875
- dense_up: bfloat16 [4096, 1024], P('ep', 'tp'), may hold values from -0.1875 to 0.1875
- dense_down: bfloat16 [4096, 1024], P('ep', 'tp'), may hold values from -0.25 to 0.25
- branch_gate: bfloat16 [1024], replicated, may hold values from -0.1875 to 0.1875
Outputs:
- layer_out: bfloat16 [128, 1024], P('ep', 'tp')
The draws below stay inside these ranges and needn't reach their ends.
Inputs may be any that keep to these rules, and one draw needn't show every extreme that they name: `expert_ids`: each row names 2 different experts. Among the rows of one device, no expert is named by more than 10 rows, and in every draw some expert is named by exactly 10 rows of some device.
All inputs are finite; a program needn't handle non-finite values.
Results may differ from the reference program's by a relative error of at most 0.02.
Values may be sent and summed in bfloat16 or wider, within the bound.
A program may use at most 64 MiB of HBM per device.

```python
import math
import jax
import jax.numpy as jnp
import numpy as np
from jax import lax

D = 1024
HEADS = 8
DK = 128
DV = 128
FF = 512
FD = 4096
TOPK = 2
SEQ_DEV = 16
SEQS = 128
EXPERTS = 8
CAP = 10
N_EP = 8
N_TP = 4


def levels(own_key, extent, split, least, largest):
    loudness = 1.0
    for axis_at, shards_of in split:
        heights = jax.random.uniform(jax.random.fold_in(jax.random.fold_in(own_key, 6), axis_at), (shards_of,), jnp.float32, least / len(split), largest / len(split))
        loudness = loudness * jnp.repeat(jnp.exp(heights), extent[axis_at] // shards_of).reshape((-1,) + (1,) * (len(extent) - 1 - axis_at))
    return loudness


def assign_block(stream_key, own, number, rows, count, top, bound, skew):
    order = jax.random.permutation(stream_key, count)
    crowded, usual = shares(count, rows * top, bound, skew, True), shares(count, rows * top, bound, skew, False)
    places = jnp.arange(count)

    def named(tallies, rotation):
        used = int((tallies > 0).sum())
        fixed = max(1, used // 4)
        shifted = fixed + (places - fixed + rotation * (used - fixed)) % max(1, count - fixed)
        return jnp.zeros((count,), jnp.int32).at[order[jnp.where(places < fixed, places, shifted)]].set(jnp.asarray(tallies, jnp.int32))

    tallies = jnp.where(number % 4 == 0, named(crowded, number // 4), named(usual, number - number // 4 - 1))
    mixed = jax.random.permutation(jax.random.fold_in(own, 3), count)
    donor, receiver = mixed[0:count // 2 * 2:2], mixed[1:count // 2 * 2:2]
    room = jnp.minimum(tallies[donor] - 1, bound - tallies[receiver]) // 2
    room = jnp.where((donor == order[0]) | (receiver == order[0]) | (tallies[receiver] == 0), 0, jnp.maximum(room, 0))
    shifted = jax.random.randint(jax.random.fold_in(own, 4), (count // 2,), 0, 1 << 20) % (room + 1)
    tallies = tallies.at[donor].add(-shifted).at[receiver].add(shifted)
    labels = jnp.searchsorted(jnp.cumsum(tallies), jnp.arange(rows * top), side="right").astype(jnp.int32)
    listing = labels.reshape(top, rows).T
    listing = listing[jax.random.permutation(jax.random.fold_in(own, 1), rows)]
    rotation = jax.random.randint(jax.random.fold_in(own, 2), (rows, 1), 0, top)
    return jnp.take_along_axis(listing, (jnp.arange(top)[None, :] + rotation) % top, axis=1)


def shares(count, total, reach, skew, full):
    loads = [(1 << 20) // math.isqrt(grade ** skew) + 1 for grade in range(1, count + 1)]
    largest = reach if full else min(reach, max(-(-total // count), total * loads[0] // sum(loads)))
    least = 1 if total - largest >= count - 1 else 0
    counts, surplus = [largest] + [least] * (count - 1), total - largest - least * (count - 1)
    while surplus > 0:
        movable = [i for i in range(1, count) if counts[i] < largest] or [i for i in range(1, count) if counts[i] < reach]
        mass, left = sum([loads[i] for i in movable]), surplus
        for i in movable:
            extra = min(reach - counts[i], max(1, left * loads[i] // mass), surplus)
            counts[i] = counts[i] + extra
            surplus = surplus - extra
    return np.array(counts)


def normal_values(stream_key, shape, scale, reach, cuts=(), kind=jnp.bfloat16):
    values = jax.random.normal(stream_key, shape, jnp.float32) * scale
    if len(cuts) > 0:
        values = levels(stream_key, shape, cuts, -0.22, 0.18) * values
    return jnp.clip(values, min=-reach, max=reach).astype(kind)


def setup_inputs(seed: int = 0) -> dict:
    arg_keys = jax.random.split(jax.random.key(seed), 23)
    hidden_in = normal_values(arg_keys[0], (SEQS, D), 1.0, 6.0, ((0, 8),))
    prior_state = normal_values(arg_keys[1], (SEQS, HEADS, DK, DV), 0.3, 4.0, ((0, 8), (1, 4)), jnp.float32)
    mix_gain = jnp.clip(1.0 + 0.18 * jax.random.normal(arg_keys[2], (D,), jnp.float32), 0.1, 1.9)
    query_w = normal_values(arg_keys[3], (D, HEADS * DK), D ** -0.5, 0.1875, ((1, 4),))
    key_w = normal_values(arg_keys[4], (D, HEADS * DK), D ** -0.5, 0.1875, ((1, 4),))
    value_w = normal_values(arg_keys[5], (D, HEADS * DV), D ** -0.5, 0.1875, ((1, 4),))
    decay_w = normal_values(arg_keys[6], (D, HEADS), D ** -0.5, 0.1875, ((1, 4),))
    beta_w = normal_values(arg_keys[7], (D, HEADS), D ** -0.5, 0.1875, ((1, 4),))
    decay_rate = jnp.clip(jnp.exp(math.log(3.0) - 4.0943445 * jax.random.uniform(arg_keys[8], (HEADS,), jnp.float32) ** levels(arg_keys[8], (HEADS,), ((0, 4),), -0.2, 0.2)), 0.05, 3.0)
    head_gain = jnp.clip(1.0 + 0.18 * jax.random.normal(arg_keys[9], (DV,), jnp.float32), 0.1, 1.9)
    out_w = normal_values(arg_keys[10], (HEADS * DV, D), (HEADS * DV) ** -0.5, 0.1875, ((0, 4),))
    ffn_gain = jnp.clip(1.0 + 0.18 * jax.random.normal(arg_keys[11], (D,), jnp.float32), 0.1, 1.9)
    expert_ids_keys = jax.random.split(jax.random.fold_in(arg_keys[12], 1), SEQS // SEQ_DEV)
    expert_ids_turns = jax.random.permutation(jax.random.fold_in(arg_keys[12], 3), SEQS // SEQ_DEV)
    expert_ids = jax.vmap(lambda own, number: assign_block(jax.random.fold_in(arg_keys[12], 2), own, number, SEQ_DEV, EXPERTS, TOPK, CAP, 2))(expert_ids_keys, expert_ids_turns).reshape((SEQS, TOPK))
    group_share = jnp.clip(0.3 + 0.7 * jax.random.uniform(arg_keys[13], (SEQS,), jnp.float32) ** levels(arg_keys[13], (SEQS,), ((0, 8),), -0.2, 0.2), 0.3, 1.0)
    expert_share = jnp.clip(0.1 + 0.9 * jax.random.uniform(arg_keys[14], (SEQS, TOPK), jnp.float32) ** levels(arg_keys[14], (SEQS, TOPK), ((0, 8),), -0.2, 0.2), 0.1, 1.0)
    expert_gate = normal_values(arg_keys[15], (EXPERTS, D, FF), D ** -0.5, 0.1875, ((0, 8), (2, 4)))
    expert_up = normal_values(arg_keys[16], (EXPERTS, D, FF), D ** -0.5, 0.1875, ((0, 8), (2, 4)))
    expert_down = normal_values(arg_keys[17], (EXPERTS, FF, D), FF ** -0.5, 0.25, ((0, 8), (1, 4)))
    dense_gate = normal_values(arg_keys[18], (FD, D), D ** -0.5, 0.1875, ((0, 8), (1, 4)))
    dense_up = normal_values(arg_keys[19], (FD, D), D ** -0.5, 0.1875, ((0, 8), (1, 4)))
    dense_down = normal_values(arg_keys[20], (FD, D), (FD // 8) ** -0.5, 0.25, ((0, 8), (1, 4)))
    branch_gate = normal_values(arg_keys[21], (D,), D ** -0.5, 0.1875)
    return {"hidden_in": hidden_in, "prior_state": prior_state, "mix_gain": mix_gain, "query_w": query_w, "key_w": key_w, "value_w": value_w, "decay_w": decay_w, "beta_w": beta_w, "decay_rate": decay_rate, "head_gain": head_gain, "out_w": out_w, "ffn_gain": ffn_gain, "expert_ids": expert_ids, "group_share": group_share, "expert_share": expert_share, "expert_gate": expert_gate, "expert_up": expert_up, "expert_down": expert_down, "dense_gate": dense_gate, "dense_up": dense_up, "dense_down": dense_down, "branch_gate": branch_gate}


def rms_scale(values, gain, floor):
    return values * lax.rsqrt(lax.optimization_barrier(jnp.mean(values * values, axis=-1, keepdims=True)) + floor) * gain

def unit_rows(values):
    return values * lax.rsqrt(lax.optimization_barrier(jnp.sum(values * values, axis=-1, keepdims=True)) + 1.0)

def delta_read(queries, key_rows, value_rows, beta_vals, decay_vals, prior_state):
    stacked = jnp.stack([queries, key_rows], axis=2)
    readout = jnp.einsum('shcd,shde->shce', stacked, prior_state, precision=lax.Precision.HIGHEST)
    intersection = lax.optimization_barrier(jnp.sum(queries * key_rows, axis=-1)) * beta_vals
    return decay_vals[..., None] * readout[:, :, 0] + intersection[..., None] * (value_rows - decay_vals[..., None] * readout[:, :, 1])

def experts_sum(normed2, expert_ids, route_weight, expert_gate, expert_up, expert_down):
    total_rows = normed2.shape[0]
    slot_total = N_EP * CAP

    def one_expert(totals, inputs):
        expert_index, w_gate, w_up, w_down = inputs
        matches = expert_ids == expert_index
        token_weight = lax.optimization_barrier(jnp.sum(jnp.where(matches, route_weight, 0.0), axis=1))
        routed = jnp.any(matches, axis=1)
        slot_rank = jnp.cumsum(routed.astype(jnp.int32)) - 1
        target = jnp.where(routed, slot_rank, slot_total).astype(jnp.int32)
        source = jnp.zeros((slot_total + 1,), jnp.int32).at[target].set(jnp.arange(total_rows, dtype=jnp.int32))[:slot_total]
        row_block = normed2[source]
        gate_pre = jnp.dot(row_block, w_gate, preferred_element_type=jnp.float32)
        up_pre = jnp.dot(row_block, w_up, preferred_element_type=jnp.float32)
        hidden = (jax.nn.silu(gate_pre) * up_pre).astype(jnp.bfloat16)
        rounded = jnp.dot(hidden, w_down, preferred_element_type=jnp.float32).astype(jnp.bfloat16)
        expert_out = lax.optimization_barrier(rounded).astype(jnp.float32)
        is_valid = jnp.arange(slot_total) < jnp.sum(routed.astype(jnp.int32))
        row_scale = jnp.where(is_valid, token_weight[source], 0.0)
        totals = totals.at[source].add(expert_out * row_scale[:, None])
        return (totals, None)
    start_sum = jnp.zeros((total_rows, normed2.shape[1]), jnp.float32)
    totals, _ = lax.scan(one_expert, start_sum, (jnp.arange(EXPERTS, dtype=jnp.int32), expert_gate, expert_up, expert_down))
    return totals

def reference(hidden_in, prior_state, mix_gain, query_w, key_w, value_w, decay_w, beta_w, decay_rate, head_gain, out_w, ffn_gain, expert_ids, group_share, expert_share, expert_gate, expert_up, expert_down, dense_gate, dense_up, dense_down, branch_gate):
    total_rows = hidden_in.shape[0]
    normed = rms_scale(hidden_in.astype(jnp.float32), mix_gain, 0.1).astype(jnp.bfloat16)
    queries = unit_rows(jnp.dot(normed, query_w, preferred_element_type=jnp.float32).reshape(total_rows, HEADS, DK))
    key_rows = unit_rows(jnp.dot(normed, key_w, preferred_element_type=jnp.float32).reshape(total_rows, HEADS, DK))
    value_rows = jnp.dot(normed, value_w, preferred_element_type=jnp.float32).reshape(total_rows, HEADS, DV)
    beta_vals = jax.nn.sigmoid(jnp.dot(normed, beta_w, preferred_element_type=jnp.float32))
    decay_vals = jnp.exp(-decay_rate * jax.nn.softplus(jnp.dot(normed, decay_w, preferred_element_type=jnp.float32)))
    readout = delta_read(queries, key_rows, value_rows, beta_vals, decay_vals, prior_state)
    head_out = rms_scale(readout, head_gain, 0.01).astype(jnp.bfloat16)
    grouped = head_out.reshape(total_rows, N_TP, HEADS * DV // N_TP).astype(jnp.float32)
    out_groups = out_w.reshape(N_TP, HEADS * DV // N_TP, D).astype(jnp.float32)
    partial_out = jnp.einsum('sgk,gkd->gsd', grouped, out_groups).astype(jnp.bfloat16)
    mix = lax.optimization_barrier(jnp.sum(partial_out.astype(jnp.float32), axis=0))
    resid = (hidden_in.astype(jnp.float32) + mix).astype(jnp.bfloat16)
    normed2 = rms_scale(resid.astype(jnp.float32), ffn_gain, 0.1).astype(jnp.bfloat16)
    route_weight = group_share[:, None] * expert_share / lax.optimization_barrier(jnp.sum(expert_share, axis=1, keepdims=True))
    moe = experts_sum(normed2, expert_ids, route_weight, expert_gate, expert_up, expert_down)
    gate_pre = jnp.dot(normed2, dense_gate.T, preferred_element_type=jnp.float32)
    up_pre = jnp.dot(normed2, dense_up.T, preferred_element_type=jnp.float32)
    branch_hidden = (jax.nn.silu(gate_pre) * up_pre).astype(jnp.bfloat16)
    branch = jnp.dot(branch_hidden, dense_down, preferred_element_type=jnp.float32)
    branch_weight = jax.nn.sigmoid(jnp.dot(normed2, branch_gate, preferred_element_type=jnp.float32))
    return (resid.astype(jnp.float32) + moe + branch_weight[:, None] * branch).astype(jnp.bfloat16)
```

```python
import functools

import jax
import jax.numpy as jnp
from jax import lax
from jax.experimental import pallas as pl
from jax.experimental.pallas import tpu as pltpu
from jax.sharding import PartitionSpec as P

MESH = pl.DeviceIdType.MESH
NT = (((1,), (1,)), ((), ()))


def rms_scale(values, gain, floor):
    return values * lax.rsqrt(jnp.mean(values * values, axis=-1, keepdims=True) + floor) * gain


def unit_rows(values):
    return values * lax.rsqrt(jnp.sum(values * values, axis=-1, keepdims=True) + 1.0)


def mm(lhs, rhs):
    return jnp.dot(lhs, rhs, preferred_element_type=jnp.float32)


def each(low, high, body):
    if high - low <= 16:
        for step in range(low, high):
            body(step)
    else:

        def looped(step, carry):
            body(step)
            return carry

        lax.fori_loop(low, high, looped, 0)


def kernel(
    n_ep,
    n_tp,
    hidden_ref,
    mix_gain_ref,
    decay_w_ref,
    beta_w_ref,
    decay_rate_ref,
    head_gain_ref,
    ffn_gain_ref,
    ids_ref,
    group_ref,
    share_ref,
    branch_gate_ref,
    state_hbm,
    query_hbm,
    key_hbm,
    value_hbm,
    out_w_hbm,
    egate_hbm,
    eup_hbm,
    edown_hbm,
    dgate_hbm,
    dup_hbm,
    ddown_hbm,
    out_ref,
    state_v,
    qkv_v,
    out_w_v,
    egu_v,
    edown_v,
    ddown_v,
    wide,
    part,
    resid_v,
    rows,
    esend,
    erecv,
    fsend,
    frecv,
    local_sem,
    wide_send,
    wide_recv,
    part_send,
    part_recv,
    rows_send,
    rows_recv,
    e_send,
    e_recv,
    f_send,
    f_recv,
):
    me_e = lax.axis_index("ep")
    me_t = lax.axis_index("tp")
    seq, width = hidden_ref.shape
    heads = state_v.shape[1]
    key_size = state_v.shape[2]
    quarter = out_ref.shape[1]

    def partner(bit):
        return me_t + bit - 2 * bit * ((me_t // bit) % 2)

    loads = []

    def load(src, dst):
        copy = pltpu.make_async_copy(src, dst, local_sem.at[len(loads)])
        copy.start()
        loads.append(copy)
        return copy

    qkv_loads = [
        load(query_hbm, qkv_v.at[0]),
        load(key_hbm, qkv_v.at[1]),
        load(value_hbm, qkv_v.at[2]),
    ]
    cut = 4 if seq % 4 == 0 else 1
    step_rows = seq // cut
    state_loads = [
        load(
            state_hbm.at[pl.ds(i * step_rows, step_rows)],
            state_v.at[pl.ds(i * step_rows, step_rows)],
        )
        for i in range(cut)
    ]
    out_load = load(out_w_hbm, out_w_v)
    barrier = pltpu.get_barrier_semaphore()

    def greet_ep(step):
        pl.semaphore_signal(
            barrier, inc=1, device_id={"ep": (me_e + step) % n_ep}, device_id_type=MESH
        )

    def greet_tp(step):
        pl.semaphore_signal(
            barrier, inc=1, device_id={"tp": (me_t + step) % n_tp}, device_id_type=MESH
        )

    each(1, n_tp, greet_tp)
    each(1, n_ep, greet_ep)
    wide_loads = [load(dgate_hbm, wide.at[0, me_t]), load(dup_hbm, wide.at[1, me_t])]
    moe_loads = [
        load(egate_hbm.at[0], egu_v.at[0]),
        load(eup_hbm.at[0], egu_v.at[1]),
        load(edown_hbm.at[0], edown_v),
    ]
    down_load = load(ddown_hbm, ddown_v)
    pl.semaphore_wait(barrier, n_ep + n_tp - 2)

    bits = []
    bit = n_tp // 2
    while bit >= 1:
        bits.append(bit)
        bit //= 2

    def wide_copy(which, src, slot, bit, index):
        return pltpu.make_async_remote_copy(
            src_ref=src,
            dst_ref=wide.at[which, slot],
            send_sem=wide_send.at[which, index],
            recv_sem=wide_recv.at[which, index],
            device_id={"tp": partner(bit)},
            device_id_type=MESH,
        )

    wide_all = ({}, {})

    def send_own(which):
        src = (dgate_hbm, dup_hbm)[which]
        for bit in bits:
            copy = wide_copy(which, src, me_t, bit, bit)
            copy.start()
            wide_all[which][bit] = copy

    def flip(value, bit):
        return value + bit - 2 * bit * ((value // bit) % 2)

    def relay(which):
        arrived = []
        for at, bit in enumerate(bits):
            fresh = [bit] + [mask + bit for mask in arrived]
            arrived = arrived + fresh
            for mask in fresh:
                if at < len(bits) - 1:
                    wide_all[which][mask].wait_recv()
                    slot = me_t
                    for one in bits:
                        if mask & one:
                            slot = flip(slot, one)
                    for lower in bits[at + 1 :]:
                        copy = wide_copy(which, wide.at[which, slot], slot, lower, mask + lower)
                        copy.start()
                        wide_all[which][mask + lower] = copy

    send_own(0)

    hidden = hidden_ref[...].astype(jnp.float32)
    normed = rms_scale(hidden, mix_gain_ref[...], 0.1).astype(jnp.bfloat16)
    beta = jax.nn.sigmoid(mm(normed, beta_w_ref[...]))
    decay_pre = mm(normed, decay_w_ref[...])
    softplus = jnp.maximum(decay_pre, 0.0) + jnp.log1p(jnp.exp(-jnp.abs(decay_pre)))
    group_row = group_ref[...]
    diagonal = lax.broadcasted_iota(jnp.int32, (seq, seq), 0) == lax.broadcasted_iota(
        jnp.int32, (seq, seq), 1
    )
    group_col = jnp.sum(
        jnp.where(diagonal, jnp.broadcast_to(group_row, (seq, seq)), 0.0), axis=1, keepdims=True
    )
    share = share_ref[...]
    ids = ids_ref[...]
    route = group_col * share / jnp.sum(share, axis=1, keepdims=True)
    pad = rows.shape[2] - width
    lanes = lax.broadcasted_iota(jnp.int32, (seq, pad), 1)
    spread = jnp.zeros((seq, pad), jnp.float32)
    for k in range(ids.shape[1]):
        spread = spread + jnp.where(ids[:, k : k + 1] == lanes, route[:, k : k + 1], 0.0)

    for copy in qkv_loads:
        copy.wait()
    queries = mm(normed, qkv_v[0])
    keys = mm(normed, qkv_v[1])
    values = mm(normed, qkv_v[2])
    row_of = lax.broadcasted_iota(jnp.int32, (seq, out_w_v.shape[0] // heads), 0)
    q_rows, k_rows, stacked = [], [], []
    for h in range(heads):
        span = slice(h * key_size, (h + 1) * key_size)
        q_rows.append(unit_rows(queries[:, span]))
        k_rows.append(unit_rows(keys[:, span]))
        stacked.append(jnp.concatenate([q_rows[h], k_rows[h]], axis=0).astype(jnp.bfloat16))
    read_q = [jnp.zeros(row_of.shape, jnp.float32) for _ in range(heads)]
    read_k = [jnp.zeros(row_of.shape, jnp.float32) for _ in range(heads)]
    for s in range(seq):
        if s % step_rows == 0:
            state_loads[s // step_rows].wait()
        for h in range(heads):
            both = mm(stacked[h], state_v[s, h].astype(jnp.bfloat16))
            read_q[h] = jnp.where(row_of == s, both[:seq], read_q[h])
            read_k[h] = jnp.where(row_of == s, both[seq:], read_k[h])
    outs = []
    value_size = row_of.shape[1]
    for h in range(heads):
        decay = jnp.exp(-decay_rate_ref[h] * softplus[:, h : h + 1])
        inner = jnp.sum(q_rows[h] * k_rows[h], axis=1, keepdims=True) * beta[:, h : h + 1]
        value_rows = values[:, h * value_size : (h + 1) * value_size]
        readout = decay * read_q[h] + inner * (value_rows - decay * read_k[h])
        outs.append(rms_scale(readout, head_gain_ref[...], 0.01).astype(jnp.bfloat16))
    out_load.wait()
    part[me_t] = mm(jnp.concatenate(outs, axis=1), out_w_v[...]).astype(jnp.bfloat16)
    part_copies = []
    for step in range(1, n_tp):
        copy = pltpu.make_async_remote_copy(
            src_ref=part.at[me_t],
            dst_ref=part.at[me_t],
            send_sem=part_send.at[step],
            recv_sem=part_recv.at[step],
            device_id={"tp": (me_t + step) % n_tp},
            device_id_type=MESH,
        )
        copy.start()
        part_copies.append(copy)
    send_own(1)
    for copy in part_copies:
        copy.wait_recv()
    mix = part[0].astype(jnp.float32)
    for t in range(1, n_tp):
        mix = mix + part[t].astype(jnp.float32)
    resid = (hidden + mix).astype(jnp.bfloat16).astype(jnp.float32)
    resid_v[...] = resid
    rows[me_e, :, :width] = rms_scale(resid, ffn_gain_ref[...], 0.1).astype(jnp.bfloat16)
    rows[me_e, :, width:] = spread.astype(jnp.bfloat16)

    def send_rows(step):
        pltpu.make_async_remote_copy(
            src_ref=rows.at[me_e],
            dst_ref=rows.at[me_e],
            send_sem=rows_send,
            recv_sem=rows_recv,
            device_id={"ep": (me_e + step) % n_ep},
            device_id_type=MESH,
        ).start()

    each(1, n_ep, send_rows)
    relay(0)
    for copy in moe_loads:
        copy.wait()

    def wait_bytes(ref, sem):
        pltpu.make_async_copy(ref, ref, sem).wait()

    wait_bytes(rows.at[pl.ds(0, n_ep - 1)], rows_recv)

    group = min(n_ep, 8)
    tall = group * seq

    def expert_block(block):
        both = rows[pl.ds(block * group, group)].reshape(tall, rows.shape[2])
        row_block = both[:, :width]
        weights = both[:, width:].astype(jnp.float32)
        mine = lax.broadcasted_iota(jnp.int32, weights.shape, 1) == me_e
        weight = jnp.sum(jnp.where(mine, weights, 0.0), axis=1, keepdims=True)
        gate = mm(row_block, egu_v[0])
        up = mm(row_block, egu_v[1])
        unit = (gate * jax.nn.sigmoid(gate) * up).astype(jnp.bfloat16)
        outs = mm(unit, edown_v[...]) * weight
        for t in range(n_tp):
            esend[t, pl.ds(block * tall, tall)] = outs[:, t * quarter : (t + 1) * quarter].astype(
                jnp.bfloat16
            )

    each(0, n_ep // group, expert_block)
    e_copies = []
    for step in range(1, n_tp):
        peer = (me_t + step) % n_tp
        copy = pltpu.make_async_remote_copy(
            src_ref=esend.at[peer],
            dst_ref=erecv.at[step - 1],
            send_sem=e_send.at[step],
            recv_sem=e_recv.at[step],
            device_id={"tp": peer},
            device_id_type=MESH,
        )
        copy.start()
        e_copies.append(copy)
    relay(1)
    for copy in wide_loads:
        copy.wait()
    down_load.wait()
    last = [mask for mask in range(1, n_tp) if mask % 2 == 1]
    for which in (0, 1):
        for mask in last:
            wide_all[which][mask].wait_recv()

    def branch_block(block):
        at = pl.ds(block * tall, tall)
        row_block = rows[pl.ds(block * group, group)].reshape(tall, rows.shape[2])[:, :width]
        gate, up = 0.0, 0.0
        for t in range(n_tp):
            piece = row_block[:, t * quarter : (t + 1) * quarter]
            gate = gate + lax.dot_general(
                piece, wide[0, t], NT, preferred_element_type=jnp.float32
            )
            up = up + lax.dot_general(piece, wide[1, t], NT, preferred_element_type=jnp.float32)
        unit = (gate * jax.nn.sigmoid(gate) * up).astype(jnp.bfloat16)
        branch = mm(unit, ddown_v[...])
        pre = jnp.sum(
            row_block.astype(jnp.float32) * branch_gate_ref[...].astype(jnp.float32),
            axis=1,
            keepdims=True,
        )
        return jax.nn.sigmoid(pre) * branch + esend[me_t, at].astype(jnp.float32)

    def store_block(block, total):
        fsend[pl.ds(block * group, group)] = total.astype(jnp.bfloat16).reshape(
            group, seq, quarter
        )

    def finish(block, total):
        at = pl.ds(block * tall, tall)
        for step in range(n_tp - 1):
            total = total + erecv[step, at].astype(jnp.float32)
        store_block(block, total)

    if n_ep == group:
        total = branch_block(0)
        for copy in e_copies:
            copy.wait_recv()
        finish(0, total)
    else:
        for copy in e_copies:
            copy.wait_recv()
        each(0, n_ep // group, lambda block: finish(block, branch_block(block)))

    def send_final(step):
        peer = (me_e + step) % n_ep
        pltpu.make_async_remote_copy(
            src_ref=fsend.at[peer],
            dst_ref=frecv.at[step - 1],
            send_sem=f_send,
            recv_sem=f_recv,
            device_id={"ep": peer},
            device_id_type=MESH,
        ).start()

    each(1, n_ep, send_final)
    mine = pl.ds(pl.multiple_of(me_t * quarter, quarter), quarter)
    total = resid_v[:, mine] + fsend[me_e].astype(jnp.float32)
    wait_bytes(frecv, f_recv)
    total = total + jnp.sum(frecv[...].astype(jnp.float32), axis=0)
    out_ref[...] = total.astype(jnp.bfloat16)
    wait_bytes(frecv, f_send)
    wait_bytes(rows.at[pl.ds(0, n_ep - 1)], rows_send)
    for copy in part_copies + e_copies:
        copy.wait_send()
    for which in (0, 1):
        for copy in wide_all[which].values():
            copy.wait_send()


def local(n_ep, n_tp, *args):
    (
        hidden_in,
        prior_state,
        mix_gain,
        query_w,
        key_w,
        value_w,
        decay_w,
        beta_w,
        decay_rate,
        head_gain,
        out_w,
        ffn_gain,
        expert_ids,
        group_share,
        expert_share,
        expert_gate,
        expert_up,
        expert_down,
        dense_gate,
        dense_up,
        dense_down,
        branch_gate,
    ) = args
    seq, width = hidden_in.shape
    quarter = width // n_tp
    tokens = n_ep * seq
    pad = -(-n_ep // 128) * 128
    vmem = pl.BlockSpec(memory_space=pltpu.VMEM)
    anywhere = pl.BlockSpec(memory_space=pl.ANY)
    bf16 = jnp.bfloat16
    dma = pltpu.SemaphoreType.DMA
    return pl.pallas_call(
        functools.partial(kernel, n_ep, n_tp),
        out_shape=jax.ShapeDtypeStruct((seq, quarter), bf16),
        in_specs=[vmem] * 4
        + [pl.BlockSpec(memory_space=pltpu.SMEM)]
        + [vmem] * 6
        + [anywhere] * 11,
        out_specs=vmem,
        scratch_shapes=[
            pltpu.VMEM(prior_state.shape, jnp.float32),
            pltpu.VMEM((3,) + query_w.shape, bf16),
            pltpu.VMEM(out_w.shape, bf16),
            pltpu.VMEM((2,) + expert_gate.shape[1:], bf16),
            pltpu.VMEM(expert_down.shape[1:], bf16),
            pltpu.VMEM(dense_down.shape, bf16),
            pltpu.VMEM((2, n_tp) + dense_gate.shape, bf16),
            pltpu.VMEM((n_tp, seq, width), bf16),
            pltpu.VMEM((seq, width), jnp.float32),
            pltpu.VMEM((n_ep, seq, width + pad), bf16),
            pltpu.VMEM((n_tp, tokens, quarter), bf16),
            pltpu.VMEM((n_tp - 1, tokens, quarter), bf16),
            pltpu.VMEM((n_ep, seq, quarter), bf16),
            pltpu.VMEM((n_ep - 1, seq, quarter), bf16),
            dma((16,)),
            dma((2, n_tp)),
            dma((2, n_tp)),
            dma((n_tp,)),
            dma((n_tp,)),
            dma,
            dma,
            dma((n_tp,)),
            dma((n_tp,)),
            dma,
            dma,
        ],
        compiler_params=pltpu.CompilerParams(
            collective_id=0, has_side_effects=True, vmem_limit_bytes=56 * 1024 * 1024
        ),
        name="layer_step",
    )(
        hidden_in,
        mix_gain[None, :],
        decay_w,
        beta_w,
        decay_rate,
        head_gain[None, :],
        ffn_gain[None, :],
        expert_ids,
        group_share[None, :],
        expert_share,
        branch_gate[None, :],
        prior_state,
        query_w,
        key_w,
        value_w,
        out_w,
        expert_gate,
        expert_up,
        expert_down,
        dense_gate,
        dense_up,
        dense_down,
    )


def solution(mesh):
    placed = (
        P("ep", None),
        P("ep", "tp", None, None),
        P(),
        P(None, "tp"),
        P(None, "tp"),
        P(None, "tp"),
        P(None, "tp"),
        P(None, "tp"),
        P("tp"),
        P(),
        P("tp", None),
        P(),
        P("ep", None),
        P("ep"),
        P("ep", None),
        P("ep", None, "tp"),
        P("ep", None, "tp"),
        P("ep", "tp", None),
        P("ep", "tp"),
        P("ep", "tp"),
        P("ep", "tp"),
        P(),
    )
    body = functools.partial(local, mesh.shape["ep"], mesh.shape["tp"])
    return jax.shard_map(
        body, mesh=mesh, in_specs=placed, out_specs=P("ep", "tp"), check_vma=False
    )
```

```python
import functools

import jax
import jax.numpy as jnp
from jax import lax
from jax.experimental import pallas as pl
from jax.experimental.pallas import tpu as pltpu
from jax.sharding import PartitionSpec as P

MESH = pl.DeviceIdType.MESH
NT = (((1,), (1,)), ((), ()))


def rms_scale(values, gain, floor):
    return values * lax.rsqrt(jnp.mean(values * values, axis=-1, keepdims=True) + floor) * gain


def unit_rows(values):
    return values * lax.rsqrt(jnp.sum(values * values, axis=-1, keepdims=True) + 1.0)


def mm(lhs, rhs):
    return jnp.dot(lhs, rhs, preferred_element_type=jnp.float32)


def mm_nt(lhs, rhs):
    return lax.dot_general(lhs, rhs, NT, preferred_element_type=jnp.float32)


def each(low, high, body):
    if high - low <= 16:
        for step in range(low, high):
            body(step)
    else:

        def looped(step, carry):
            body(step)
            return carry

        lax.fori_loop(low, high, looped, 0)


def kernel(
    n_ep,
    n_tp,
    hidden_ref,
    mix_gain_ref,
    decay_w_ref,
    beta_w_ref,
    decay_rate_ref,
    head_gain_ref,
    ffn_gain_ref,
    ids_ref,
    group_ref,
    share_ref,
    branch_gate_ref,
    state_hbm,
    query_hbm,
    key_hbm,
    value_hbm,
    out_w_hbm,
    egate_hbm,
    eup_hbm,
    edown_hbm,
    dgate_hbm,
    dup_hbm,
    ddown_hbm,
    out_ref,
    state_v,
    qkv_v,
    out_w_v,
    egu_v,
    edown_v,
    ddown_v,
    wide,
    part,
    resid_v,
    rows,
    wts,
    esend,
    erecv,
    fsend,
    frecv,
    local_sem,
    wide_send,
    wide_recv,
    part_send,
    part_recv,
    rows_send,
    rows_recv,
    half_send,
    half_recv,
    wts_send,
    wts_recv,
    e_send,
    e_recv,
    f_send,
    f_recv,
):
    me_e = lax.axis_index("ep")
    me_t = lax.axis_index("tp")
    seq, width = hidden_ref.shape
    heads = state_v.shape[1]
    key_size = state_v.shape[2]
    quarter = out_ref.shape[1]

    def partner(bit):
        return me_t + bit - 2 * bit * ((me_t // bit) % 2)

    loads = []

    def load(src, dst):
        copy = pltpu.make_async_copy(src, dst, local_sem.at[len(loads)])
        copy.start()
        loads.append(copy)
        return copy

    qkv_loads = [
        load(query_hbm, qkv_v.at[0]),
        load(key_hbm, qkv_v.at[1]),
        load(value_hbm, qkv_v.at[2]),
    ]
    cut = 4 if seq % 4 == 0 else 1
    step_rows = seq // cut
    state_loads = [
        load(
            state_hbm.at[pl.ds(i * step_rows, step_rows)],
            state_v.at[pl.ds(i * step_rows, step_rows)],
        )
        for i in range(cut)
    ]
    out_load = load(out_w_hbm, out_w_v)
    barrier = pltpu.get_barrier_semaphore()

    def greet_ep(step):
        pl.semaphore_signal(
            barrier, inc=1, device_id={"ep": (me_e + step) % n_ep}, device_id_type=MESH
        )

    def greet_tp(step):
        pl.semaphore_signal(
            barrier, inc=1, device_id={"tp": (me_t + step) % n_tp}, device_id_type=MESH
        )

    each(1, n_tp, greet_tp)
    each(1, n_ep, greet_ep)
    wide_loads = [load(dgate_hbm, wide.at[0, me_t]), load(dup_hbm, wide.at[1, me_t])]
    moe_loads = [
        load(egate_hbm.at[0], egu_v.at[0]),
        load(eup_hbm.at[0], egu_v.at[1]),
        load(edown_hbm.at[0], edown_v),
    ]
    down_load = load(ddown_hbm, ddown_v)
    pl.semaphore_wait(barrier, n_ep + n_tp - 2)

    bits = []
    bit = n_tp // 2
    while bit >= 1:
        bits.append(bit)
        bit //= 2

    def wide_copy(which, src, slot, bit, index):
        return pltpu.make_async_remote_copy(
            src_ref=src,
            dst_ref=wide.at[which, slot],
            send_sem=wide_send.at[which, index],
            recv_sem=wide_recv.at[which, index],
            device_id={"tp": partner(bit)},
            device_id_type=MESH,
        )

    wide_all = ({}, {})

    def send_own(which):
        src = wide.at[which, me_t]
        wide_loads[which].wait()
        for bit in bits:
            copy = wide_copy(which, src, me_t, bit, bit)
            copy.start()
            wide_all[which][bit] = copy

    def flip(value, bit):
        return value + bit - 2 * bit * ((value // bit) % 2)

    def relay(which):
        arrived = []
        for at, bit in enumerate(bits):
            fresh = [bit] + [mask + bit for mask in arrived]
            arrived = arrived + fresh
            for mask in fresh:
                if at < len(bits) - 1:
                    wide_all[which][mask].wait_recv()
                    slot = me_t
                    for one in bits:
                        if mask & one:
                            slot = flip(slot, one)
                    for lower in bits[at + 1 :]:
                        copy = wide_copy(which, wide.at[which, slot], slot, lower, mask + lower)
                        copy.start()
                        wide_all[which][mask + lower] = copy


    hidden = hidden_ref[...].astype(jnp.float32)
    normed = rms_scale(hidden, mix_gain_ref[...], 0.1).astype(jnp.bfloat16)
    beta = jax.nn.sigmoid(mm_nt(normed, beta_w_ref[...]))
    decay_pre = mm_nt(normed, decay_w_ref[...])
    softplus = jnp.maximum(decay_pre, 0.0) + jnp.log1p(jnp.exp(-jnp.abs(decay_pre)))
    diagonal = lax.broadcasted_iota(jnp.int32, (seq, seq), 0) == lax.broadcasted_iota(
        jnp.int32, (seq, seq), 1
    )

    def column(row):
        spread_row = jnp.broadcast_to(row, (seq, seq))
        return jnp.sum(jnp.where(diagonal, spread_row, jnp.zeros_like(spread_row)), axis=1, keepdims=True)

    share = share_ref[...]
    ids = ids_ref[...]
    route = group_ref[...] * share / jnp.sum(share, axis=0, keepdims=True)
    pad = wts.shape[2]
    lanes = lax.broadcasted_iota(jnp.int32, (seq, pad), 1)
    spread = jnp.zeros((seq, pad), jnp.float32)
    for k in range(ids.shape[0]):
        spread = spread + jnp.where(column(ids[k : k + 1]) == lanes, column(route[k : k + 1]), 0.0)

    wts[me_e] = spread

    def send_weights(step):
        pltpu.make_async_remote_copy(
            src_ref=wts.at[me_e],
            dst_ref=wts.at[me_e],
            send_sem=wts_send,
            recv_sem=wts_recv,
            device_id={"ep": (me_e + step) % n_ep},
            device_id_type=MESH,
        ).start()

    each(1, n_ep, send_weights)
    for copy in qkv_loads:
        copy.wait()
    queries = mm(normed, qkv_v[0])
    keys = mm(normed, qkv_v[1])
    values = mm(normed, qkv_v[2])
    row_of = lax.broadcasted_iota(jnp.int32, (seq, out_w_v.shape[0] // heads), 0)
    q_rows, k_rows, stacked = [], [], []
    for h in range(heads):
        span = slice(h * key_size, (h + 1) * key_size)
        q_rows.append(unit_rows(queries[:, span]))
        k_rows.append(unit_rows(keys[:, span]))
        stacked.append(jnp.concatenate([q_rows[h], k_rows[h]], axis=0).astype(jnp.bfloat16))
    read_q = [jnp.zeros(row_of.shape, jnp.float32) for _ in range(heads)]
    read_k = [jnp.zeros(row_of.shape, jnp.float32) for _ in range(heads)]
    for s in range(seq):
        if s % step_rows == 0:
            state_loads[s // step_rows].wait()
        for h in range(heads):
            both = mm(stacked[h], state_v[s, h].astype(jnp.bfloat16))
            read_q[h] = jnp.where(row_of == s, both[:seq], read_q[h])
            read_k[h] = jnp.where(row_of == s, both[seq:], read_k[h])
    outs = []
    value_size = row_of.shape[1]
    for h in range(heads):
        decay = jnp.exp(-decay_rate_ref[h] * softplus[:, h : h + 1])
        inner = jnp.sum(q_rows[h] * k_rows[h], axis=1, keepdims=True) * beta[:, h : h + 1]
        value_rows = values[:, h * value_size : (h + 1) * value_size]
        readout = decay * read_q[h] + inner * (value_rows - decay * read_k[h])
        outs.append(rms_scale(readout, head_gain_ref[...], 0.01).astype(jnp.bfloat16))
    out_load.wait()
    part[me_t] = mm(jnp.concatenate(outs, axis=1), out_w_v[...]).astype(jnp.bfloat16)
    part_copies = []
    for step in range(1, n_tp):
        copy = pltpu.make_async_remote_copy(
            src_ref=part.at[me_t],
            dst_ref=part.at[me_t],
            send_sem=part_send.at[step],
            recv_sem=part_recv.at[step],
            device_id={"tp": (me_t + step) % n_tp},
            device_id_type=MESH,
        )
        copy.start()
        part_copies.append(copy)
    send_own(0)
    send_own(1)
    for copy in part_copies:
        copy.wait_recv()
    mix = part[0].astype(jnp.float32)
    for t in range(1, n_tp):
        mix = mix + part[t].astype(jnp.float32)
    resid = (hidden + mix).astype(jnp.bfloat16).astype(jnp.float32)
    resid_v[...] = resid
    normed2 = rms_scale(resid, ffn_gain_ref[...], 0.1)
    half = me_t % 2
    half_width = width // 2
    rows[half, me_e] = jnp.where(
        half == 0, normed2[:, :half_width], normed2[:, half_width:]
    ).astype(jnp.bfloat16)

    def send_rows(step):
        pltpu.make_async_remote_copy(
            src_ref=rows.at[half, me_e],
            dst_ref=rows.at[half, me_e],
            send_sem=rows_send,
            recv_sem=rows_recv,
            device_id={"ep": (me_e + step) % n_ep},
            device_id_type=MESH,
        ).start()

    each(1, n_ep, send_rows)
    relay(0)
    for copy in moe_loads:
        copy.wait()

    def wait_bytes(ref, sem):
        pltpu.make_async_copy(ref, ref, sem).wait()

    wait_bytes(rows.at[half, pl.ds(0, n_ep - 1)], rows_recv)
    half_copy = pltpu.make_async_remote_copy(
        src_ref=rows.at[half],
        dst_ref=rows.at[half],
        send_sem=half_send,
        recv_sem=half_recv,
        device_id={"tp": partner(1)},
        device_id_type=MESH,
    )
    half_copy.start()
    wait_bytes(wts.at[pl.ds(0, n_ep - 1)], wts_recv)
    half_copy.wait_recv()

    group = min(n_ep, 8)
    tall = group * seq

    def token_rows(block):
        at = pl.ds(block * group, group)
        return jnp.concatenate(
            [rows[side, at].reshape(tall, half_width) for side in (0, 1)], axis=1
        )

    def expert_block(block):
        row_block = token_rows(block)
        weights = wts[pl.ds(block * group, group)].reshape(tall, wts.shape[2])
        mine = lax.broadcasted_iota(jnp.int32, weights.shape, 1) == me_e
        weight = jnp.sum(jnp.where(mine, weights, 0.0), axis=1, keepdims=True)
        gate = mm(row_block, egu_v[0])
        up = mm(row_block, egu_v[1])
        unit = (gate * jax.nn.sigmoid(gate) * up).astype(jnp.bfloat16)
        outs = mm(unit, edown_v[...]) * weight
        for t in range(n_tp):
            esend[t, pl.ds(block * tall, tall)] = outs[:, t * quarter : (t + 1) * quarter].astype(
                jnp.bfloat16
            )

    each(0, n_ep // group, expert_block)
    e_copies = []
    for step in range(1, n_tp):
        peer = (me_t + step) % n_tp
        copy = pltpu.make_async_remote_copy(
            src_ref=esend.at[peer],
            dst_ref=erecv.at[step - 1],
            send_sem=e_send.at[step],
            recv_sem=e_recv.at[step],
            device_id={"tp": peer},
            device_id_type=MESH,
        )
        copy.start()
        e_copies.append(copy)
    down_load.wait()

    def wait_wide(which):
        for mask in range(1, n_tp, 2):
            wide_all[which][mask].wait_recv()

    def term(row_block, which):
        total = 0.0
        for t in range(n_tp):
            piece = row_block[:, t * quarter : (t + 1) * quarter]
            total = total + lax.dot_general(
                piece, wide[which, t], NT, preferred_element_type=jnp.float32
            )
        return total

    def branch_weight(row_block):
        products = 0.0
        lane = branch_gate_ref.shape[1]
        for c in range(branch_gate_ref.shape[0]):
            piece = row_block[:, c * lane : (c + 1) * lane].astype(jnp.float32)
            products = products + piece * branch_gate_ref[c : c + 1].astype(jnp.float32)
        return jax.nn.sigmoid(jnp.sum(products, axis=1, keepdims=True))

    def branch_block(block, row_block, gate, scale):
        at = pl.ds(block * tall, tall)
        gate = gate * jax.nn.sigmoid(gate)
        up = term(row_block, 1)
        unit = (gate * up).astype(jnp.bfloat16)
        branch = mm(unit, ddown_v[...])
        return scale * branch + esend[me_t, at].astype(jnp.float32)

    def store_block(block, total):
        fsend[pl.ds(block * group, group)] = total.astype(jnp.bfloat16).reshape(
            group, seq, quarter
        )

    def finish(block, total):
        at = pl.ds(block * tall, tall)
        for step in range(n_tp - 1):
            total = total + erecv[step, at].astype(jnp.float32)
        store_block(block, total)

    wait_wide(0)
    if n_ep == group:
        row_block = token_rows(0)
        gate = term(row_block, 0)
        scale = branch_weight(row_block)
        relay(1)
        wait_wide(1)
        total = branch_block(0, row_block, gate, scale)
        for copy in e_copies:
            copy.wait_recv()
        finish(0, total)
    else:
        relay(1)
        wait_wide(1)
        for copy in e_copies:
            copy.wait_recv()

        def whole_block(block):
            row_block = token_rows(block)
            scale = branch_weight(row_block)
            finish(block, branch_block(block, row_block, term(row_block, 0), scale))

        each(0, n_ep // group, whole_block)

    def send_final(step):
        peer = (me_e + step) % n_ep
        pltpu.make_async_remote_copy(
            src_ref=fsend.at[peer],
            dst_ref=frecv.at[step - 1],
            send_sem=f_send,
            recv_sem=f_recv,
            device_id={"ep": peer},
            device_id_type=MESH,
        ).start()

    each(1, n_ep, send_final)
    mine = pl.ds(pl.multiple_of(me_t * quarter, quarter), quarter)
    total = resid_v[:, mine] + fsend[me_e].astype(jnp.float32)
    wait_bytes(frecv, f_recv)
    total = total + jnp.sum(frecv[...].astype(jnp.float32), axis=0)
    out_ref[...] = total.astype(jnp.bfloat16)
    wait_bytes(frecv, f_send)
    wait_bytes(rows.at[half, pl.ds(0, n_ep - 1)], rows_send)
    wait_bytes(wts.at[pl.ds(0, n_ep - 1)], wts_send)
    half_copy.wait_send()
    for copy in part_copies + e_copies:
        copy.wait_send()
    for which in (0, 1):
        for copy in wide_all[which].values():
            copy.wait_send()


def local(n_ep, n_tp, *args):
    (
        hidden_in,
        prior_state,
        mix_gain,
        query_w,
        key_w,
        value_w,
        decay_w,
        beta_w,
        decay_rate,
        head_gain,
        out_w,
        ffn_gain,
        expert_ids,
        group_share,
        expert_share,
        expert_gate,
        expert_up,
        expert_down,
        dense_gate,
        dense_up,
        dense_down,
        branch_gate,
    ) = args
    seq, width = hidden_in.shape
    quarter = width // n_tp
    tokens = n_ep * seq
    pad = -(-n_ep // 128) * 128
    vmem = pl.BlockSpec(memory_space=pltpu.VMEM)
    anywhere = pl.BlockSpec(memory_space=pl.ANY)
    bf16 = jnp.bfloat16
    dma = pltpu.SemaphoreType.DMA
    return pl.pallas_call(
        functools.partial(kernel, n_ep, n_tp),
        out_shape=jax.ShapeDtypeStruct((seq, quarter), bf16),
        in_specs=[vmem] * 4
        + [pl.BlockSpec(memory_space=pltpu.SMEM)]
        + [vmem] * 6
        + [anywhere] * 11,
        out_specs=vmem,
        scratch_shapes=[
            pltpu.VMEM(prior_state.shape, jnp.float32),
            pltpu.VMEM((3,) + query_w.shape, bf16),
            pltpu.VMEM(out_w.shape, bf16),
            pltpu.VMEM((2,) + expert_gate.shape[1:], bf16),
            pltpu.VMEM(expert_down.shape[1:], bf16),
            pltpu.VMEM(dense_down.shape, bf16),
            pltpu.VMEM((2, n_tp) + dense_gate.shape, bf16),
            pltpu.VMEM((n_tp, seq, width), bf16),
            pltpu.VMEM((seq, width), jnp.float32),
            pltpu.VMEM((2, n_ep, seq, width // 2), bf16),
            pltpu.VMEM((n_ep, seq, pad), jnp.float32),
            pltpu.VMEM((n_tp, tokens, quarter), bf16),
            pltpu.VMEM((n_tp - 1, tokens, quarter), bf16),
            pltpu.VMEM((n_ep, seq, quarter), bf16),
            pltpu.VMEM((n_ep - 1, seq, quarter), bf16),
            dma((16,)),
            dma((2, n_tp)),
            dma((2, n_tp)),
            dma((n_tp,)),
            dma((n_tp,)),
            dma,
            dma,
            dma,
            dma,
            dma,
            dma,
            dma((n_tp,)),
            dma((n_tp,)),
            dma,
            dma,
        ],
        compiler_params=pltpu.CompilerParams(
            collective_id=0, has_side_effects=True, vmem_limit_bytes=56 * 1024 * 1024
        ),
        name="layer_step",
    )(
        hidden_in,
        mix_gain[None, :],
        decay_w.T,
        beta_w.T,
        decay_rate,
        head_gain[None, :],
        ffn_gain[None, :],
        expert_ids.T,
        group_share[None, :],
        expert_share.T,
        branch_gate.reshape(width // 128, 128),
        prior_state,
        query_w,
        key_w,
        value_w,
        out_w,
        expert_gate,
        expert_up,
        expert_down,
        dense_gate,
        dense_up,
        dense_down,
    )


def solution(mesh):
    placed = (
        P("ep", None),
        P("ep", "tp", None, None),
        P(),
        P(None, "tp"),
        P(None, "tp"),
        P(None, "tp"),
        P(None, "tp"),
        P(None, "tp"),
        P("tp"),
        P(),
        P("tp", None),
        P(),
        P("ep", None),
        P("ep"),
        P("ep", None),
        P("ep", None, "tp"),
        P("ep", None, "tp"),
        P("ep", "tp", None),
        P("ep", "tp"),
        P("ep", "tp"),
        P("ep", "tp"),
        P(),
    )
    body = functools.partial(local, mesh.shape["ep"], mesh.shape["tp"])
    return jax.shard_map(
        body, mesh=mesh, in_specs=placed, out_specs=P("ep", "tp"), check_vma=False
    )
```
